32 devices in a mesh: sp: 8 (over z, x), tp: 4 (over y, core).
Axes of the slice: x: 2, y: 2, z: 4, core: 2. Of those that a mesh axis runs over, the one named last changes fastest.
Arguments:
- pool_input: bfloat16 [2048, 256], P('sp', 'tp'), may hold values from -6 to 6
- pool_weight: bfloat16 [4, 64, 64], P('tp'), may hold values from -0.75 to 0.75
- pool_gain: bfloat16 [256], P('tp'), may hold values from 0.099609375 to 1.8984375
- out_weight: bfloat16 [256, 2048], P(None, 'tp'), may hold values from -0.375 to 0.375
- resid: bfloat16 [2048, 2048], P('sp', 'tp'), may hold values from -90 to 90
- norm_gain: bfloat16 [2048], P('tp'), may hold values from 0.099609375 to 1.8984375
- routes: int32 [2048, 2], P('sp'), may hold values from 0 to 7, all different within a row; in each aligned block of 256 rows (0 to 255, 256 to 511, ...) at most 128 rows name the same one
- route_weight: float32 [2048, 2], P('sp'), may hold values from 0.2 to 1
- expert_gate: bfloat16 [8, 2048, 4096], P('sp', None, 'tp'), may hold values from -0.375 to 0.375
- expert_up: bfloat16 [8, 2048, 4096], P('sp', None, 'tp'), may hold values from -0.375 to 0.375
- expert_down: bfloat16 [8, 4096, 2048], P('sp', 'tp'), may hold values from -0.0234375 to 0.0234375
Outputs:
- layer_out: bfloat16 [2048, 2048], P('sp', 'tp')
The draws below stay inside these ranges and needn't reach their ends.
Inputs may be any that keep to these rules, and one draw needn't show every extreme that they name: `routes`: the 2 experts of a position differ. In each aligned block of 256 positions no expert is named by more than 128 assignments; some block reaches that bound.
All inputs are finite; a program needn't handle non-finite values.
Results may differ from the reference program's by a relative error of at most 0.0085.
Values may be sent and summed in bfloat16 or wider, within the bound.
A program may use at most 64 MiB of HBM per device.

```python
import math
from functools import partial
import jax
import jax.numpy as jnp
import numpy as np
from jax import lax

D = 2048
FF = 4096
GSIZE = 64
REACH = 16
TOPK = 2
TOK_SP = 256
GROUPS = 4
PW = 256
EXPERTS = 8
CAP = 128
TOKENS = 2048
N_SP = 8
N_TP = 4


def draw_resid(key, part):
    key_jitter, key_rows = jax.random.split(key, 2)
    column = 0.3 * 10.0 ** (jnp.arange(D, dtype=jnp.float32) / D)
    jitter = jnp.clip(jax.random.normal(key_jitter, (TOKENS, D), jnp.float32), -6.0, 6.0)
    spread = jax.random.uniform(key_rows, (TOKENS, 1), jnp.float32, 0.0, 0.5)
    return (jitter * column * 10.0 ** spread).astype(jnp.bfloat16)


def spiked(values, stream_key, source, target, parts, factor):
    def block_of(dim):
        return (jnp.arange(values.shape[dim]) // (values.shape[dim] // parts)).reshape((-1,) + (1,) * (values.ndim - 1 - dim))

    near = jax.random.permutation(stream_key, parts)[block_of(target)]
    other_side = (block_of(target) + parts // 2) % parts
    return jnp.where((block_of(source) == near) | (block_of(source) == other_side), factor * values, values)


def block_levels(key, shape, pieces, smallest, largest):
    gain, own = 1.0, jax.random.fold_in(key, 6)
    for dim, shards_of in pieces:
        draws = jnp.exp(jax.random.uniform(jax.random.fold_in(own, dim), (shards_of,), jnp.float32, smallest / len(pieces), largest / len(pieces)))
        gain = gain * jnp.repeat(draws, shape[dim] // shards_of).reshape([-1 if axis == dim else 1 for axis in range(len(shape))])
    return gain


def routed_block(own_key, own, number, rows, amount, top, bound, slope):
    sequence = jax.random.permutation(own_key, amount)
    crowded, usual = shares(amount, rows * top, bound, slope, True), shares(amount, rows * top, bound, slope, False)
    places = jnp.arange(amount)

    def named(lengths, turn):
        used = int((lengths > 0).sum())
        fixed = max(1, used // 4)
        passed = fixed + (places - fixed + turn * (used - fixed)) % max(1, amount - fixed)
        return jnp.zeros((amount,), jnp.int32).at[sequence[jnp.where(places < fixed, places, passed)]].set(jnp.asarray(lengths, jnp.int32))

    lengths = jnp.where(number % 4 == 0, named(crowded, number // 4), named(usual, number - number // 4 - 1))
    mixed = jax.random.permutation(jax.random.fold_in(own, 3), amount)
    donor, receiver = mixed[0:amount // 2 * 2:2], mixed[1:amount // 2 * 2:2]
    margin = jnp.minimum(lengths[donor] - 1, bound - lengths[receiver]) // 2
    margin = jnp.where((donor == sequence[0]) | (receiver == sequence[0]) | (lengths[receiver] == 0), 0, jnp.maximum(margin, 0))
    passed = jax.random.randint(jax.random.fold_in(own, 4), (amount // 2,), 0, 1 << 20) % (margin + 1)
    lengths = lengths.at[donor].add(-passed).at[receiver].add(passed)
    items = jnp.searchsorted(jnp.cumsum(lengths), jnp.arange(rows * top), side="right").astype(jnp.int32)
    listing = items.reshape(top, rows).T
    listing = listing[jax.random.permutation(jax.random.fold_in(own, 1), rows)]
    turn = jax.random.randint(jax.random.fold_in(own, 2), (rows, 1), 0, top)
    return jnp.take_along_axis(listing, (jnp.arange(top)[None, :] + turn) % top, axis=1)


def shares(amount, total, bound, skew, full):
    weights = [(1 << 20) // math.isqrt(rank ** skew) + 1 for rank in range(1, amount + 1)]
    largest = bound if full else min(bound, max(-(-total // amount), total * weights[0] // sum(weights)))
    least = 1 if total - largest >= amount - 1 else 0
    holding, surplus = [largest] + [least] * (amount - 1), total - largest - least * (amount - 1)
    while surplus > 0:
        movable = [i for i in range(1, amount) if holding[i] < largest] or [i for i in range(1, amount) if holding[i] < bound]
        mass, remaining = sum([weights[i] for i in movable]), surplus
        for i in movable:
            more = min(bound - holding[i], max(1, remaining * weights[i] // mass), surplus)
            holding[i] = holding[i] + more
            surplus = surplus - more
    return np.array(holding)


def bell_draw(key, shape, scale, limit, pieces=(), kind=jnp.bfloat16):
    factor_of = block_levels(key, shape, pieces, -0.22, 0.18) if pieces else 1.0
    entries = jax.random.normal(key, shape, jnp.float32) * scale * factor_of
    return jnp.minimum(jnp.maximum(entries, -limit), limit).astype(kind)


def heavy_noise(own_key, extent, scale, most, cuts, heavy, held_as=jnp.bfloat16):
    entries = scale * jax.random.normal(own_key, extent, jnp.float32)
    if cuts:
        entries = entries * block_levels(own_key, extent, cuts, -0.22, 0.18)
    return jnp.clip(spiked(entries, jax.random.fold_in(own_key, 3), *heavy), -most, most).astype(held_as)


def setup_inputs(seed: int = 0) -> dict:
    arg_keys = jax.random.split(jax.random.key(seed), 12)
    pool_input = bell_draw(arg_keys[0], (TOKENS, PW), 1.0, 6.0, ((0, 8), (1, 4)))
    pool_weight = bell_draw(arg_keys[1], (GROUPS, GSIZE, GSIZE), GSIZE ** -0.5, 0.75, ((0, 4),))
    pool_gain = jnp.clip(1.0 + 0.18 * jax.random.normal(arg_keys[2], (PW,), jnp.float32), 0.099609375, 1.8984375).astype(jnp.bfloat16)
    out_weight = bell_draw(arg_keys[3], (PW, D), PW ** -0.5, 0.375, ((1, 4),))
    resid = draw_resid(jax.random.fold_in(arg_keys[11], 71), 0)
    norm_gain = jnp.clip(1.0 + 0.18 * jax.random.normal(arg_keys[5], (D,), jnp.float32), 0.099609375, 1.8984375).astype(jnp.bfloat16)
    routes_keys = jax.random.split(jax.random.fold_in(arg_keys[6], 1), TOKENS // TOK_SP)
    routes_turns = jax.random.permutation(jax.random.fold_in(arg_keys[6], 3), TOKENS // TOK_SP)
    routes = jax.vmap(lambda own, number: routed_block(jax.random.fold_in(arg_keys[6], 2), own, number, TOK_SP, EXPERTS, TOPK, CAP, 1))(routes_keys, routes_turns).reshape((TOKENS, TOPK))
    route_weight = jnp.clip(0.2 + 0.8 * jax.random.uniform(arg_keys[7], (TOKENS, TOPK), jnp.float32) ** block_levels(arg_keys[7], (TOKENS, TOPK), ((0, 8),), -0.2, 0.2), 0.2, 1.0)
    expert_gate = bell_draw(arg_keys[8], (EXPERTS, D, FF), (D // 9) ** -0.5, 0.375, ((0, 8), (2, 4)))
    expert_up = bell_draw(arg_keys[9], (EXPERTS, D, FF), (D // 9) ** -0.5, 0.375, ((0, 8), (2, 4)))
    expert_down = heavy_noise(arg_keys[10], (EXPERTS, FF, D), (FF * 32) ** -0.5, 0.0234375, ((0, 8), (1, 4)), (1, 2, 4, 2.0))
    return {"pool_input": pool_input, "pool_weight": pool_weight, "pool_gain": pool_gain, "out_weight": out_weight, "resid": resid, "norm_gain": norm_gain, "routes": routes, "route_weight": route_weight, "expert_gate": expert_gate, "expert_up": expert_up, "expert_down": expert_down}


GATE_LIMIT = 7.0
GATE_ALPHA = 1.702
NORM_EPS = 1e-05

def clamped_unit(gate_pre, up_pre):
    gate_cut = jnp.minimum(gate_pre, GATE_LIMIT)
    up_cut = jnp.clip(up_pre, -GATE_LIMIT, GATE_LIMIT)
    return (up_cut + 1.0) * gate_cut * jax.nn.sigmoid(GATE_ALPHA * gate_cut)

def window_pool(extended, width_of, position, tok_count):
    summed = jnp.zeros((tok_count, extended.shape[1]), jnp.float32)
    for offset in range(REACH):
        first_row = REACH - 1 - offset
        shifted = extended[first_row:first_row + tok_count]
        summed = summed + jnp.where(offset < width_of[None, :], shifted, 0.0)
    counted = jnp.minimum(position[:, None] + 1, width_of[None, :]).astype(jnp.float32)
    current = extended[REACH - 1:]
    return (summed / counted - current).astype(jnp.bfloat16)

def slot_of(route_block, expert_count, capacity):
    flattened = route_block.reshape(-1).astype(jnp.int32)
    onehot = (flattened[:, None] == jnp.arange(expert_count, dtype=jnp.int32)[None, :]).astype(jnp.int32)
    earlier = (jnp.cumsum(onehot, axis=0) - onehot).astype(jnp.int32)
    ranked = lax.optimization_barrier(jnp.sum(earlier * onehot, axis=1)).astype(jnp.int32)
    return (flattened * capacity + ranked).astype(jnp.int32)

def fill_table(slot_row, id_row, weight_row):
    id_table = jnp.full((EXPERTS * CAP,), TOKENS, jnp.int32).at[slot_row].set(id_row)
    weight_table = jnp.zeros((EXPERTS * CAP,), jnp.float32).at[slot_row].set(weight_row)
    return (id_table, weight_table)

def reference(pool_input, pool_weight, pool_gain, out_weight, resid, norm_gain, routes, route_weight, expert_gate, expert_up, expert_down):
    channels = pool_input.shape[1]
    width_of = 2 ** (1 + jnp.arange(channels, dtype=jnp.int32) // GSIZE % 4)
    position = jnp.arange(TOKENS, dtype=jnp.int32)
    extended = jnp.concatenate([jnp.zeros((REACH - 1, channels), jnp.float32), pool_input.astype(jnp.float32)], axis=0)
    pooled = window_pool(extended, width_of, position, TOKENS)
    grouped = jnp.einsum('tgc,gcd->tgd', pooled.reshape(TOKENS, GROUPS, GSIZE).astype(jnp.float32), pool_weight.astype(jnp.float32))
    mixed_out = (grouped * pool_gain.astype(jnp.float32).reshape(GROUPS, GSIZE)).astype(jnp.bfloat16).reshape(TOKENS, PW)
    projected = jnp.dot(mixed_out, out_weight, preferred_element_type=jnp.float32)
    stored = lax.optimization_barrier((resid.astype(jnp.float32) + projected).astype(jnp.bfloat16))
    stream = stored.astype(jnp.float32)
    scale_row = lax.rsqrt(lax.optimization_barrier(jnp.mean(stream * stream, axis=1, keepdims=True)) + NORM_EPS)
    normed = (stream * scale_row * norm_gain.astype(jnp.float32)).astype(jnp.bfloat16)
    slots = jax.vmap(partial(slot_of, expert_count=EXPERTS, capacity=CAP))(routes.reshape(N_SP, TOK_SP, TOPK))
    token_ids = jnp.repeat(jnp.arange(TOKENS, dtype=jnp.int32), TOPK).reshape(N_SP, TOK_SP * TOPK)
    weights = route_weight.astype(jnp.float32).reshape(N_SP, TOK_SP * TOPK)
    id_tables, weight_tables = jax.vmap(fill_table)(slots, token_ids, weights)
    id_tables = id_tables.reshape(N_SP, EXPERTS, CAP).transpose(1, 0, 2).reshape(EXPERTS, N_SP * CAP)
    weight_tables = weight_tables.reshape(N_SP, EXPERTS, CAP).transpose(1, 0, 2).reshape(EXPERTS, N_SP * CAP)
    hidden_part = FF // N_TP

    def expert_step(running, inputs):
        id_row, weight_row, gate_w, up_w, down_w = inputs
        chosen = jnp.take(normed, id_row, axis=0, mode='fill', fill_value=0)
        gate_pre = jnp.dot(chosen, gate_w, preferred_element_type=jnp.float32)
        up_pre = jnp.dot(chosen, up_w, preferred_element_type=jnp.float32)
        hidden = clamped_unit(gate_pre, up_pre).astype(jnp.bfloat16)
        summed = jnp.zeros((id_row.shape[0], D), jnp.float32)
        for block_idx in range(N_TP):
            lower = block_idx * hidden_part
            partial_out = jnp.dot(hidden[:, lower:lower + hidden_part], down_w[lower:lower + hidden_part], preferred_element_type=jnp.float32)
            rounded = lax.optimization_barrier(partial_out.astype(jnp.bfloat16))
            summed = summed + rounded.astype(jnp.float32)
        output_rows = lax.optimization_barrier(summed.astype(jnp.bfloat16)).astype(jnp.float32)
        running = running.at[id_row].add(output_rows * weight_row[:, None], mode='drop')
        return (running, None)
    running, ignored = lax.scan(expert_step, jnp.zeros((TOKENS, D), jnp.float32), (id_tables, weight_tables, expert_gate, expert_up, expert_down))
    return (stream + running).astype(jnp.bfloat16)
```

```python
import functools

import jax
import jax.numpy as jnp
from jax import lax
from jax.experimental import pallas as pl
from jax.experimental.pallas import tpu as pltpu
from jax.sharding import PartitionSpec as P

GSIZE = 64
REACH = 16
TOPK = 2
CORES = 2
LANES = 128
CHUNK_ROWS = 128
EARLY = 3

GATE_LIMIT = 7.0
GATE_ALPHA = 1.702
NORM_EPS = 1e-05

F32 = jnp.float32
BF16 = jnp.bfloat16
MESH = pl.DeviceIdType.MESH


def dot(a, b):
    return jnp.dot(a, b, preferred_element_type=F32)


def visiting_order(n):
    far = [(j / max(1, n // 2), d) for j, d in enumerate(range(n // 2, n)) if d > 1]
    near = [((j + 0.9) / max(1, n // 2 - 2), d) for j, d in enumerate(range(2, n // 2))]
    return list(range(min(n, 2))) + [d for _, d in sorted(far + near)]


def flipped(index, bits):
    bit = 1
    while bit <= bits:
        if bits & bit:
            index = index + bit * (1 - 2 * lax.rem(index // bit, 2))
        bit *= 2
    return index


def windows(summed, level):
    rows, channels = summed.shape
    window, span = jnp.zeros((rows - REACH, channels), F32), jnp.zeros((1, channels), F32)
    for power in range(4):
        summed = summed + pltpu.roll(summed, 1 << power, 0)
        window = jnp.where(level == power, summed[REACH:], window)
        span = jnp.where(level == power, float(2 << power), span)
    return window, span


def layer_kernel(
    n, tp, cap,
    pool_ref, mix_ref, gain_ref, proj_ref, resid_ref, norm_ref, routes_ref, weight_ref, gate_hbm, up_hbm, down_hbm,
    out_ref,
    edge, edges, packed, squares, stream_ref, normed_ref,
    x, sent, row_send, row_recv, wg, wu, wd, hidden, own, mine, pc_send, pc_recv, ys_send, ys_recv, res, ret, acc,
    w_sem, h_send, h_recv, m_send, m_recv, s_send, s_recv, g_send, g_recv, a_send, a_recv, b_send, b_recv, c_send, c_recv, d_send, d_recv, e_send, e_recv, f_send, f_recv,
):
    ny = tp // CORES
    tok, feat = resid_ref.shape
    channels = pool_ref.shape[0]
    model, width = wg.shape
    group = x.shape[0] // ys_send.shape[0]
    chunks = n // group
    rows = group * cap
    order = visiting_order(n)
    sp = lax.axis_index("sp")
    t = lax.axis_index("tp")
    y, core = t // CORES, t % CORES
    partner = y * CORES + (1 - core)
    other = [flipped(sp, d) for d in order]

    loads = [
        pltpu.make_async_copy(gate_hbm.at[0], wg, w_sem.at[0]),
        pltpu.make_async_copy(up_hbm.at[0], wu, w_sem.at[1]),
        pltpu.make_async_copy(down_hbm.at[0], wd, w_sem.at[2]),
    ]
    for load in loads:
        load.start()

    barrier = pltpu.get_barrier_semaphore()
    after, before = lax.rem(sp + 1, n), lax.rem(sp + n - 1, n)
    peers = [(other[i], t) for i in range(1, n)]
    peers += [(sp, lax.rem(t + k, tp)) for k in range(1, tp)]
    peers += [(s, lax.rem(t + k, tp)) for s in (after, before) for k in range(1, tp)]
    for peer in peers:
        pl.semaphore_signal(barrier, inc=1, device_id=peer, device_id_type=MESH)

    def cols(block):
        return pl.ds(pl.multiple_of(block * feat, LANES), feat)

    def remote(src, dst, send, recv, device):
        return pltpu.make_async_remote_copy(
            src_ref=src, dst_ref=dst, send_sem=send, recv_sem=recv, device_id=device, device_id_type=MESH
        )

    def copy_a(i):
        return remote(sent.at[i], x.at[i, :, cols(t)], a_send.at[i], a_recv.at[i], (other[i], t))

    def copy_g(i):
        return remote(row_send.at[i], row_recv.at[i], g_send.at[i], g_recv.at[i], (other[i], t))

    def copy_b(i, k):
        part = x.at[i, :, cols(t)]
        return remote(part, part, b_send.at[i, k], b_recv.at[i, k], (sp, lax.rem(y + k, ny) * CORES + core))

    def copy_c(i, k):
        part = x.at[i, :, cols(lax.rem(y + ny - k, ny) * CORES + core)]
        return remote(part, part, c_send.at[i, k], c_recv.at[i, k], (sp, partner))

    def copy_d(q):
        return remote(pc_send.at[q], pc_recv.at[q], d_send.at[q], d_recv.at[q], (sp, partner))

    def copy_e(q, k):
        return remote(
            ys_send.at[q, k], ys_recv.at[q, k], e_send.at[q, k], e_recv.at[q, k],
            (sp, lax.rem(y + k, ny) * CORES + core),
        )

    def copy_f(i):
        return remote(res.at[i], ret.at[i], f_send.at[i], f_recv.at[i], (other[i], t))

    def copy_h(k):
        return remote(edge, edges.at[k], h_send.at[k], h_recv.at[k], (after, lax.rem(t + k, tp)))

    def copy_m(k):
        return remote(packed.at[0], packed.at[k], m_send.at[k], m_recv.at[k], (sp, lax.rem(t + k, tp)))

    def copy_s(k):
        return remote(squares.at[0], squares.at[k], s_send.at[k], s_recv.at[k], (sp, lax.rem(t + k, tp)))

    with jax.named_scope("local"):
        current = pool_ref[...].astype(F32).T
        groups = channels // GSIZE
        group_of = t * groups + lax.broadcasted_iota(jnp.int32, (1, channels), 1) // GSIZE
        level = lax.rem(group_of, 4)
        blank = jnp.zeros((REACH, channels), F32)
        window, span = windows(jnp.concatenate([blank, current], axis=0), level)
        place = (sp * tok + 1 + lax.broadcasted_iota(jnp.int32, (tok, channels), 0)).astype(F32)
        pooled = (window / jnp.minimum(place, span) - current).astype(BF16)
        carried, _ = windows(jnp.concatenate([current[tok - REACH :], blank], axis=0), level)
        carried = (carried / span).astype(BF16)
        gain = gain_ref[...].astype(F32)

        def mix(values):
            parts = [dot(values[:, g * GSIZE : (g + 1) * GSIZE], mix_ref[g]) for g in range(groups)]
            return (jnp.concatenate(parts, axis=1) * gain).astype(BF16)

        mixed = mix(pooled)
        folds = max(1, LANES // channels)
        short = tok // folds
        packed[0] = jnp.concatenate([mixed[i * short : (i + 1) * short] for i in range(folds)], axis=1)
        edge[...] = jnp.concatenate([mix(carried)] * folds, axis=1)

        listed = jnp.concatenate(
            [routes_ref[...].astype(F32), weight_ref[...], jnp.zeros((8 - 2 * TOPK, tok), F32)], axis=0
        ).T
        routes = [listed[:, k : k + 1] for k in range(TOPK)]
        weights = [listed[:, TOPK + k : TOPK + k + 1] for k in range(TOPK)]
        lane = lax.broadcasted_iota(jnp.int32, (tok, LANES), 1).astype(F32)
        onehot = [jnp.where(route == lane, 1.0, 0.0) for route in routes]
        below = lax.broadcasted_iota(jnp.int32, (tok, tok), 1) < lax.broadcasted_iota(jnp.int32, (tok, tok), 0)
        earlier = dot(jnp.where(below, 1.0, 0.0).astype(BF16), sum(onehot).astype(BF16))
        keys = [
            routes[k] * float(cap) + jnp.sum(earlier * onehot[k], axis=1, keepdims=True) for k in range(TOPK)
        ]
        slot = lax.broadcasted_iota(jnp.int32, (tok, cap), 1)
        acc[...] = resid_ref[...].astype(F32)

    with jax.named_scope("barrier"):
        pl.semaphore_wait(barrier, len(peers))
    for k in range(1, tp):
        copy_m(k).start()

    @pl.when(sp < n - 1)
    def _():
        for k in range(tp):
            copy_h(k).start()

    def projected(block, k):
        first = lax.rem(t + tp - k, tp) * channels
        return dot(block, proj_ref[pl.ds(pl.multiple_of(first, GSIZE), channels), :])

    def unpacked(k):
        block = packed[k]
        return jnp.concatenate([block[:, i * channels : (i + 1) * channels] for i in range(folds)], axis=0)

    with jax.named_scope("proj"):
        acc[...] += projected(unpacked(0), 0)
        for k in range(1, tp):
            copy_m(k).wait_recv()
            acc[...] += projected(unpacked(k), k)

    with jax.named_scope("halo"):
        @pl.when(sp > 0)
        def _():
            for k in range(tp):
                copy_h(k).wait_recv()
                acc[:REACH] += projected(edges[k][:, :channels], k)

    with jax.named_scope("stream"):
        stream_ref[...] = acc[...].astype(BF16)
        stream = stream_ref[...].astype(F32)
        power = jnp.sum(stream * stream, axis=1, keepdims=True)
        squares[0] = jnp.broadcast_to(power, (tok, LANES)).T[:8]
        for k in range(1, tp):
            copy_s(k).start()
        normed_ref[...] = (stream * norm_ref[...].astype(F32)).astype(BF16)

    def chosen(i):
        wanted = (slot + other[i] * cap).astype(F32)
        return sum(jnp.where(key == wanted, 1.0, 0.0) for key in keys)

    def rows_for(i):
        return lax.dot_general(
            chosen(i).astype(BF16), normed_ref[...], (((0,), (0,)), ((), ())), preferred_element_type=F32
        ).astype(BF16)

    def arrive_a(i):
        if i:
            copy_a(i).wait_recv()
        for k in range(1, ny):
            copy_b(i, k).start()
        copy_c(i, 0).start()

    def arrive_b(i):
        for k in range(1, ny):
            copy_b(i, k).wait_recv()
            copy_c(i, k).start()

    def arrive_c(i):
        for k in range(ny):
            copy_c(i, k).wait_recv()

    def dispatch(first, last):
        for i in range(first, last):
            sent[i] = rows_for(i)
            copy_a(i).start()

    with jax.named_scope("dispatch"):
        x[0, :, cols(t)] = rows_for(0)
        arrive_a(0)
        early = min(n, 1 + EARLY)
        dispatch(1, early)

    with jax.named_scope("scales"):
        total = squares[0]
        for k in range(1, tp):
            copy_s(k).wait_recv()
            total = total + squares[k]
        scale = lax.rsqrt(total.T[:, :1] / model + NORM_EPS)
        for i in range(n):
            line = jnp.sum(chosen(i) * scale, axis=0, keepdims=True)
            if cap < LANES:
                line = jnp.concatenate([line, jnp.zeros((1, LANES - cap), F32)], axis=1)
            if i:
                row_send[i] = jnp.broadcast_to(line, row_send.shape[1:])
                copy_g(i).start()
            else:
                row_recv[0] = jnp.broadcast_to(line, row_send.shape[1:])
        dispatch(early, n)

    def finish(q):
        total = mine[q]
        for k in range(1, ny):
            copy_e(q, k).wait_recv()
            total = total + ys_recv[q, k].astype(F32)
        total = total.astype(BF16)
        for j in range(group):
            i = q * group + j
            block = total[j * cap : (j + 1) * cap]
            if i:
                res[i] = block
                copy_f(i).start()
            else:
                ret[0] = block

    def members(q):
        return range(q * group, (q + 1) * group) if q < chunks else ()

    with jax.named_scope("ahead"):
        for i in members(0):
            if i:
                arrive_a(i)
        for i in members(1):
            arrive_a(i)
        for i in members(0):
            arrive_b(i)
    for q in range(chunks):
        with jax.named_scope("wait_a"):
            for i in members(q + 2):
                arrive_a(i)
        with jax.named_scope("wait_b"):
            for i in members(q + 1):
                arrive_b(i)
        with jax.named_scope("wait_c"):
            for i in members(q):
                arrive_c(i)
                if i:
                    copy_g(i).wait_recv()
            scaled = jnp.concatenate([row_recv[i].T[:cap, :1] for i in members(q)], axis=0)
            if q == 0:
                loads[0].wait()
                loads[1].wait()

        with jax.named_scope("gateup"):
            step = min(width, 256)

            @pl.loop(0, width // step)
            def _(j):
                part = pl.ds(pl.multiple_of(j * step, LANES), step)
                block = x[q * group : (q + 1) * group].reshape(rows, model)
                gate = jnp.minimum(dot(block, wg[:, part]) * scaled, GATE_LIMIT)
                up = jnp.clip(dot(block, wu[:, part]) * scaled, -GATE_LIMIT, GATE_LIMIT)
                hidden[:, part] = ((up + 1.0) * gate * jax.nn.sigmoid(GATE_ALPHA * gate)).astype(BF16)

        with jax.named_scope("down"):
            if q == 0:
                loads[2].wait()
            for k in range(ny):
                block = lax.rem(y + k, ny) * CORES + (1 - core)
                pc_send[q, :, k * feat : (k + 1) * feat] = dot(hidden[...], wd[:, cols(block)]).astype(BF16)
            copy_d(q).start()
            for k in range(ny):
                block = lax.rem(y + k, ny) * CORES + core
                own[:, k * feat : (k + 1) * feat] = dot(hidden[...], wd[:, cols(block)])
        with jax.named_scope("finish"):
            if q:
                finish(q - 1)
        with jax.named_scope("wait_d"):
            copy_d(q).wait_recv()
            for k in range(1, ny):
                part = slice(k * feat, (k + 1) * feat)
                ys_send[q, k] = (own[:, part] + pc_recv[q, :, part].astype(F32)).astype(BF16)
                copy_e(q, k).start()
            mine[q] = own[:, :feat] + pc_recv[q, :, :feat].astype(F32)
    with jax.named_scope("finish"):
        finish(chunks - 1)

    heads = [weight.astype(BF16).astype(F32) for weight in weights]
    rests = [weights[k] - heads[k] for k in range(TOPK)]
    acc[...] = stream_ref[...].astype(F32)
    for i in range(n):
        with jax.named_scope("combine"):
            if i:
                copy_f(i).wait_recv()
            wanted = (slot + other[i] * cap).astype(F32)
            high = sum(jnp.where(keys[k] == wanted, heads[k], 0.0) for k in range(TOPK))
            low = sum(jnp.where(keys[k] == wanted, rests[k], 0.0) for k in range(TOPK))
            block = ret[i]
            acc[...] += dot(high.astype(BF16), block) + dot(low.astype(BF16), block)
    out_ref[...] = acc[...].astype(BF16)

    @pl.when(sp < n - 1)
    def _():
        for k in range(tp):
            copy_h(k).wait_send()

    for k in range(1, tp):
        copy_m(k).wait_send()
        copy_s(k).wait_send()
    for i in range(n):
        if i:
            copy_a(i).wait_send()
            copy_g(i).wait_send()
            copy_f(i).wait_send()
        for k in range(ny):
            if k:
                copy_b(i, k).wait_send()
            copy_c(i, k).wait_send()
    for q in range(chunks):
        copy_d(q).wait_send()
        for k in range(1, ny):
            copy_e(q, k).wait_send()


def on_device(
    pool_input, pool_weight, pool_gain, out_weight, resid, norm_gain,
    routes, route_weight, expert_gate, expert_up, expert_down,
):
    n, tp = lax.axis_size("sp"), lax.axis_size("tp")
    tok, feat = resid.shape
    channels = pool_input.shape[1]
    folds = max(1, LANES // channels)
    model, width = expert_gate.shape[1:]
    cap = 2 * tok * TOPK // n
    ny = tp // CORES
    group = min(n, max(1, CHUNK_ROWS // cap))
    chunks = n // group
    rows = group * cap
    sems = pltpu.SemaphoreType.DMA
    vmem = pl.BlockSpec(memory_space=pltpu.VMEM)
    hbm = pl.BlockSpec(memory_space=pl.ANY)
    return pl.pallas_call(
        functools.partial(layer_kernel, n, tp, cap),
        out_shape=jax.ShapeDtypeStruct((tok, feat), BF16),
        in_specs=[vmem] * 8 + [hbm] * 3,
        out_specs=vmem,
        scratch_shapes=[
            pltpu.VMEM((REACH, folds * channels), BF16),
            pltpu.VMEM((tp, REACH, folds * channels), BF16),
            pltpu.VMEM((tp, tok // folds, folds * channels), BF16),
            pltpu.VMEM((tp, 8, tok), F32),
            pltpu.VMEM((tok, feat), BF16),
            pltpu.VMEM((tok, feat), BF16),
            pltpu.VMEM((n, cap, model), BF16),
            pltpu.VMEM((n, cap, feat), BF16),
            pltpu.VMEM((n, 8, max(cap, LANES)), F32),
            pltpu.VMEM((n, 8, max(cap, LANES)), F32),
            pltpu.VMEM((model, width), BF16),
            pltpu.VMEM((model, width), BF16),
            pltpu.VMEM((width, model), BF16),
            pltpu.VMEM((rows, width), BF16),
            pltpu.VMEM((rows, ny * feat), F32),
            pltpu.VMEM((chunks, rows, feat), F32),
            pltpu.VMEM((chunks, rows, ny * feat), BF16),
            pltpu.VMEM((chunks, rows, ny * feat), BF16),
            pltpu.VMEM((chunks, ny, rows, feat), BF16),
            pltpu.VMEM((chunks, ny, rows, feat), BF16),
            pltpu.VMEM((n, cap, feat), BF16),
            pltpu.VMEM((n, cap, feat), BF16),
            pltpu.VMEM((tok, feat), F32),
            sems((3,)),
            sems((tp,)), sems((tp,)),
            sems((tp,)), sems((tp,)),
            sems((tp,)), sems((tp,)),
            sems((n,)), sems((n,)),
            sems((n,)), sems((n,)),
            sems((n, ny)), sems((n, ny)),
            sems((n, ny)), sems((n, ny)),
            sems((chunks,)), sems((chunks,)),
            sems((chunks, ny)), sems((chunks, ny)),
            sems((n,)), sems((n,)),
        ],
        compiler_params=pltpu.CompilerParams(
            collective_id=0, has_side_effects=True, vmem_limit_bytes=56 * 1024 * 1024
        ),
    )(
        pool_input.T, pool_weight, pool_gain.reshape(1, -1), out_weight, resid, norm_gain.reshape(1, -1),
        routes.T, route_weight.T, expert_gate, expert_up, expert_down,
    )


def solution(mesh):
    in_specs = (
        P("sp", "tp"),
        P("tp", None, None),
        P("tp"),
        P(None, "tp"),
        P("sp", "tp"),
        P("tp"),
        P("sp", None),
        P("sp", None),
        P("sp", None, "tp"),
        P("sp", None, "tp"),
        P("sp", "tp", None),
    )
    return jax.shard_map(on_device, mesh=mesh, in_specs=in_specs, out_specs=P("sp", "tp"), check_vma=False)
```

```python
import functools

import jax
import jax.numpy as jnp
from jax import lax
from jax.experimental import pallas as pl
from jax.experimental.pallas import tpu as pltpu
from jax.sharding import PartitionSpec as P

GSIZE = 64
REACH = 16
TOPK = 2
CORES = 2
LANES = 128
CHUNK_ROWS = 128
EARLY = 3

VISITS = (0, 1, 4, 3, 5, 6, 7, 2)
SENDS = (1, 2, 3, 4, 7, 5, 6)
STEPS = (
    ("relay", 0), ("gather", 1), ("gate_a", 0), ("gather", 2), ("gate_b", 0), ("down_theirs", 0), ("down_own", 0),
    ("gather", 3), ("pair", 0), ("relay", 1), ("gate_a", 1), ("gate_b", 1), ("reduce", 0), ("relay", 2),
    ("down_theirs", 1), ("down_own", 1), ("gate_a", 2), ("gather", 4), ("gate_b", 2), ("down_theirs", 2),
    ("gather", 7), ("relay", 3), ("pair", 1), ("down_own", 2), ("relay", 4), ("gather", 5), ("gate_a", 3),
    ("pair", 2), ("gate_b", 3), ("down_theirs", 3), ("reduce", 2), ("finish", 0), ("down_own", 3), ("gate_a", 4),
    ("gather", 6), ("gate_b", 4), ("relay", 5), ("down_theirs", 4), ("down_own", 4), ("gate_a", 5), ("finish", 2),
    ("pair", 4), ("reduce", 4), ("gate_b", 5), ("relay", 6), ("down_theirs", 5), ("pair", 3), ("reduce", 3),
    ("down_own", 5), ("relay", 7), ("combine", 0), ("gate_a", 6), ("finish", 4), ("pair", 5), ("reduce", 5),
    ("gate_b", 6), ("reduce", 1), ("down_theirs", 6), ("down_own", 6), ("pair", 6), ("finish", 3), ("gate_a", 7),
    ("gate_b", 7), ("down_theirs", 7), ("reduce", 6), ("finish", 5), ("down_own", 7), ("finish", 1), ("pair", 7),
    ("reduce", 7), ("finish", 6), ("combine", 3), ("combine", 4), ("combine", 1), ("finish", 7), ("combine", 2),
    ("combine", 5), ("combine", 6), ("combine", 7),
)

GATE_LIMIT = 7.0
GATE_ALPHA = 1.702
NORM_EPS = 1e-05

F32 = jnp.float32
BF16 = jnp.bfloat16
MESH = pl.DeviceIdType.MESH


def dot(a, b):
    return jnp.dot(a, b, preferred_element_type=F32)


def visiting_order(chunks, group):
    order, sends, steps = VISITS, SENDS, STEPS
    if chunks != len(VISITS):
        order, sends, steps = range(chunks), range(1, chunks), [("relay", 0)]
        for q in range(chunks):
            steps += [(name, p) for name, p in (("gather", q + 1), ("relay", q + 1)) if p < chunks]
            steps += [(name, q) for name in ("gate_a", "gate_b", "down_theirs", "down_own", "pair", "reduce")]
        steps += [("finish", q) for q in range(chunks)] + [("combine", q) for q in range(chunks)]
    offsets = [q * group + j for q in order for j in range(group)]
    sending = [*range(1, group)] + [q * group + j for q in sends for j in range(group)]
    return offsets, sending, steps


def flipped(index, bits):
    bit = 1
    while bit <= bits:
        if bits & bit:
            index = index + bit * (1 - 2 * lax.rem(index // bit, 2))
        bit *= 2
    return index


def windows(summed, level):
    rows, channels = summed.shape
    window, span = jnp.zeros((rows - REACH, channels), F32), jnp.zeros((1, channels), F32)
    for power in range(4):
        summed = summed + pltpu.roll(summed, 1 << power, 0)
        window = jnp.where(level == power, summed[REACH:], window)
        span = jnp.where(level == power, float(2 << power), span)
    return window, span


def layer_kernel(
    n, tp, cap,
    pool_ref, mix_ref, gain_ref, proj_ref, resid_ref, norm_ref, routes_ref, weight_ref, gate_hbm, up_hbm, down_hbm,
    out_ref,
    edge, edges, packed, squares, stream_ref, normed_ref,
    x, sent, row_send, row_recv, wg, wu, wd, hidden, own, mine, pc_send, pc_recv, ys_send, ys_recv, res, ret, acc,
    w_sem, h_send, h_recv, m_send, m_recv, s_send, s_recv, g_send, g_recv, a_send, a_recv, b_send, b_recv, c_send, c_recv, d_send, d_recv, e_send, e_recv, f_send, f_recv,
):
    ny = tp // CORES
    tok, feat = resid_ref.shape
    channels = pool_ref.shape[0]
    model, width = wg.shape
    group = x.shape[0] // ys_send.shape[0]
    chunks = n // group
    rows = group * cap
    order, sending, steps = visiting_order(chunks, group)
    early = group - 1 + EARLY * group
    sp = lax.axis_index("sp")
    t = lax.axis_index("tp")
    y, core = t // CORES, t % CORES
    partner = y * CORES + (1 - core)
    other = [flipped(sp, d) for d in order]

    loads = [
        pltpu.make_async_copy(gate_hbm.at[0], wg, w_sem.at[0]),
        pltpu.make_async_copy(up_hbm.at[0], wu, w_sem.at[1]),
        pltpu.make_async_copy(down_hbm.at[0], wd, w_sem.at[2]),
    ]
    for load in loads:
        load.start()

    barrier = pltpu.get_barrier_semaphore()
    after, before = lax.rem(sp + 1, n), lax.rem(sp + n - 1, n)
    peers = [(other[i], t) for i in range(1, n)]
    peers += [(sp, lax.rem(t + k, tp)) for k in range(1, tp)]
    peers += [(s, lax.rem(t + k, tp)) for s in (after, before) for k in range(1, tp)]
    for peer in peers:
        pl.semaphore_signal(barrier, inc=1, device_id=peer, device_id_type=MESH)

    def cols(block):
        return pl.ds(pl.multiple_of(block * feat, LANES), feat)

    def remote(src, dst, send, recv, device):
        return pltpu.make_async_remote_copy(
            src_ref=src, dst_ref=dst, send_sem=send, recv_sem=recv, device_id=device, device_id_type=MESH
        )

    def copy_a(i):
        return remote(sent.at[i], x.at[i, :, cols(t)], a_send.at[i], a_recv.at[i], (other[i], t))

    def copy_g(i):
        return remote(row_send.at[i], row_recv.at[i], g_send.at[i], g_recv.at[i], (other[i], t))

    def copy_b(i, k):
        part = x.at[i, :, cols(t)]
        return remote(part, part, b_send.at[i, k], b_recv.at[i, k], (sp, lax.rem(y + k, ny) * CORES + core))

    def copy_c(i, k):
        part = x.at[i, :, cols(lax.rem(y + ny - k, ny) * CORES + core)]
        return remote(part, part, c_send.at[i, k], c_recv.at[i, k], (sp, partner))

    def copy_d(q):
        return remote(pc_send.at[q], pc_recv.at[q], d_send.at[q], d_recv.at[q], (sp, partner))

    def copy_e(q, k):
        return remote(
            ys_send.at[q, k], ys_recv.at[q, k], e_send.at[q, k], e_recv.at[q, k],
            (sp, lax.rem(y + k, ny) * CORES + core),
        )

    def copy_f(i):
        return remote(res.at[i], ret.at[i], f_send.at[i], f_recv.at[i], (other[i], t))

    def copy_h(k):
        return remote(edge, edges.at[k], h_send.at[k], h_recv.at[k], (after, lax.rem(t + k, tp)))

    def copy_m(k):
        return remote(packed.at[0], packed.at[k], m_send.at[k], m_recv.at[k], (sp, lax.rem(t + k, tp)))

    def copy_s(k):
        return remote(squares.at[0], squares.at[k], s_send.at[k], s_recv.at[k], (sp, lax.rem(t + k, tp)))

    with jax.named_scope("local"):
        current = pool_ref[...].astype(F32).T
        groups = channels // GSIZE
        group_of = t * groups + lax.broadcasted_iota(jnp.int32, (1, channels), 1) // GSIZE
        level = lax.rem(group_of, 4)
        blank = jnp.zeros((REACH, channels), F32)
        window, span = windows(jnp.concatenate([blank, current], axis=0), level)
        place = (sp * tok + 1 + lax.broadcasted_iota(jnp.int32, (tok, channels), 0)).astype(F32)
        pooled = (window / jnp.minimum(place, span) - current).astype(BF16)
        carried, _ = windows(jnp.concatenate([current[tok - REACH :], blank], axis=0), level)
        carried = (carried / span).astype(BF16)
        gain = gain_ref[...].astype(F32)

        def mix(values):
            parts = [dot(values[:, g * GSIZE : (g + 1) * GSIZE], mix_ref[g]) for g in range(groups)]
            return (jnp.concatenate(parts, axis=1) * gain).astype(BF16)

        mixed = mix(pooled)
        folds = max(1, LANES // channels)
        short = tok // folds
        packed[0] = jnp.concatenate([mixed[i * short : (i + 1) * short] for i in range(folds)], axis=1)
        edge[...] = jnp.concatenate([mix(carried)] * folds, axis=1)

        listed = jnp.concatenate(
            [routes_ref[...].astype(F32), weight_ref[...], jnp.zeros((8 - 2 * TOPK, tok), F32)], axis=0
        ).T
        routes = [listed[:, k : k + 1] for k in range(TOPK)]
        weights = [listed[:, TOPK + k : TOPK + k + 1] for k in range(TOPK)]
        lane = lax.broadcasted_iota(jnp.int32, (tok, LANES), 1).astype(F32)
        onehot = [jnp.where(route == lane, 1.0, 0.0) for route in routes]
        below = lax.broadcasted_iota(jnp.int32, (tok, tok), 1) < lax.broadcasted_iota(jnp.int32, (tok, tok), 0)
        earlier = dot(jnp.where(below, 1.0, 0.0).astype(BF16), sum(onehot).astype(BF16))
        keys = [
            routes[k] * float(cap) + jnp.sum(earlier * onehot[k], axis=1, keepdims=True) for k in range(TOPK)
        ]
        slot = lax.broadcasted_iota(jnp.int32, (tok, cap), 1)
        acc[...] = resid_ref[...].astype(F32)

    with jax.named_scope("barrier"):
        pl.semaphore_wait(barrier, len(peers))
    for k in range(1, tp):
        copy_m(k).start()

    @pl.when(sp < n - 1)
    def _():
        for k in range(tp):
            copy_h(k).start()

    def projected(block, k):
        first = lax.rem(t + tp - k, tp) * channels
        return dot(block, proj_ref[pl.ds(pl.multiple_of(first, GSIZE), channels), :])

    def unpacked(k):
        block = packed[k]
        return jnp.concatenate([block[:, i * channels : (i + 1) * channels] for i in range(folds)], axis=0)

    with jax.named_scope("proj"):
        acc[...] += projected(unpacked(0), 0)
        for k in range(1, tp):
            copy_m(k).wait_recv()
            acc[...] += projected(unpacked(k), k)

    with jax.named_scope("halo"):
        @pl.when(sp > 0)
        def _():
            for k in range(tp):
                copy_h(k).wait_recv()
                acc[:REACH] += projected(edges[k][:, :channels], k)

    with jax.named_scope("stream"):
        stream_ref[...] = acc[...].astype(BF16)
        stream = stream_ref[...].astype(F32)
        power = jnp.sum(stream * stream, axis=1, keepdims=True)
        squares[0] = jnp.broadcast_to(power, (tok, LANES)).T[:8]
        for k in range(1, tp):
            copy_s(k).start()
        scaling = norm_ref[...].astype(F32)
        scaling = jnp.concatenate([scaling[i : i + 1] for i in range(feat // LANES)], axis=1)
        normed_ref[...] = (stream * scaling).astype(BF16)

    def chosen(i):
        wanted = (slot + other[i] * cap).astype(F32)
        return sum(jnp.where(key == wanted, 1.0, 0.0) for key in keys)

    def rows_for(i):
        return lax.dot_general(
            chosen(i).astype(BF16), normed_ref[...], (((0,), (0,)), ((), ())), preferred_element_type=F32
        ).astype(BF16)

    def arrive_a(i):
        if i:
            copy_a(i).wait_recv()
        for k in range(1, ny):
            copy_b(i, k).start()
        copy_c(i, 0).start()

    def arrive_b(i):
        for k in range(1, ny):
            copy_b(i, k).wait_recv()
            copy_c(i, k).start()

    def arrive_c(i):
        for k in range(ny):
            copy_c(i, k).wait_recv()

    def dispatch(first, last):
        for i in sending[first:last]:
            sent[i] = rows_for(i)
            copy_a(i).start()

    with jax.named_scope("dispatch"):
        x[0, :, cols(t)] = rows_for(0)
        arrive_a(0)
        dispatch(0, early)

    with jax.named_scope("scales"):
        total = squares[0]
        for k in range(1, tp):
            copy_s(k).wait_recv()
            total = total + squares[k]
        scale = lax.rsqrt(total.T[:, :1] / model + NORM_EPS)
        for i in range(n):
            line = jnp.sum(chosen(i) * scale, axis=0, keepdims=True)
            if cap < LANES:
                line = jnp.concatenate([line, jnp.zeros((1, LANES - cap), F32)], axis=1)
            if i:
                row_send[i] = jnp.broadcast_to(line, row_send.shape[1:])
                copy_g(i).start()
            else:
                row_recv[0] = jnp.broadcast_to(line, row_send.shape[1:])
        dispatch(early, n)

    def members(q):
        return range(q * group, (q + 1) * group) if q < chunks else ()

    def gather(q):
        for i in members(q):
            arrive_a(i)

    def relay(q):
        for i in members(q):
            arrive_b(i)

    step = min(width, 256)

    def gate_up(q, first, last):
        scaled = jnp.concatenate([row_recv[i].T[:cap, :1] for i in members(q)], axis=0)

        @pl.loop(first, last)
        def _(j):
            part = pl.ds(pl.multiple_of(j * step, LANES), step)
            block = x[q * group : (q + 1) * group].reshape(rows, model)
            gate = jnp.minimum(dot(block, wg[:, part]) * scaled, GATE_LIMIT)
            up = jnp.clip(dot(block, wu[:, part]) * scaled, -GATE_LIMIT, GATE_LIMIT)
            hidden[:, part] = ((up + 1.0) * gate * jax.nn.sigmoid(GATE_ALPHA * gate)).astype(BF16)

    def gate_a(q):
        for i in members(q):
            arrive_c(i)
            if i:
                copy_g(i).wait_recv()
        if q == 0:
            loads[0].wait()
            loads[1].wait()
        gate_up(q, 0, width // step // 2)

    def gate_b(q):
        gate_up(q, width // step // 2, width // step)

    def down_theirs(q):
        if q == 0:
            loads[2].wait()
        for k in range(ny):
            block = lax.rem(y + k, ny) * CORES + (1 - core)
            pc_send[q, :, k * feat : (k + 1) * feat] = dot(hidden[...], wd[:, cols(block)]).astype(BF16)
        copy_d(q).start()

    def down_own(q):
        for k in range(ny):
            block = lax.rem(y + k, ny) * CORES + core
            own[q % 2, :, k * feat : (k + 1) * feat] = dot(hidden[...], wd[:, cols(block)])

    def pair(q):
        copy_d(q).wait_recv()
        for k in range(1, ny):
            part = slice(k * feat, (k + 1) * feat)
            ys_send[q, k] = (own[q % 2, :, part] + pc_recv[q, :, part].astype(F32)).astype(BF16)
        mine[q] = own[q % 2, :, :feat] + pc_recv[q, :, :feat].astype(F32)

    def reduce(q):
        for k in range(1, ny):
            copy_e(q, k).start()

    def finish(q):
        total = mine[q]
        for k in range(1, ny):
            copy_e(q, k).wait_recv()
            total = total + ys_recv[q, k].astype(F32)
        total = total.astype(BF16)
        for j in range(group):
            i = q * group + j
            block = total[j * cap : (j + 1) * cap]
            if i:
                res[i] = block
                copy_f(i).start()
            else:
                ret[0] = block

    heads = [weight.astype(BF16).astype(F32) for weight in weights]
    rests = [weights[k] - heads[k] for k in range(TOPK)]

    def combine(q):
        for i in members(q):
            if i:
                copy_f(i).wait_recv()
            wanted = (slot + other[i] * cap).astype(F32)
            high = sum(jnp.where(keys[k] == wanted, heads[k], 0.0) for k in range(TOPK))
            low = sum(jnp.where(keys[k] == wanted, rests[k], 0.0) for k in range(TOPK))
            block = ret[i]
            acc[...] += dot(high.astype(BF16), block) + dot(low.astype(BF16), block)

    acc[...] = stream_ref[...].astype(F32)
    actions = dict(
        gather=gather, relay=relay, gate_a=gate_a, gate_b=gate_b, down_theirs=down_theirs, down_own=down_own,
        pair=pair, reduce=reduce, finish=finish, combine=combine,
    )
    for i in members(0):
        if i:
            arrive_a(i)
    for name, q in steps:
        with jax.named_scope(name + str(q)):
            actions[name](q)
    with jax.named_scope("out"):
        out_ref[...] = acc[...].astype(BF16)

    @pl.when(sp < n - 1)
    def _():
        for k in range(tp):
            copy_h(k).wait_send()

    for k in range(1, tp):
        copy_m(k).wait_send()
        copy_s(k).wait_send()
    for i in range(n):
        if i:
            copy_a(i).wait_send()
            copy_g(i).wait_send()
            copy_f(i).wait_send()
        for k in range(ny):
            if k:
                copy_b(i, k).wait_send()
            copy_c(i, k).wait_send()
    for q in range(chunks):
        copy_d(q).wait_send()
        for k in range(1, ny):
            copy_e(q, k).wait_send()


def on_device(
    pool_input, pool_weight, pool_gain, out_weight, resid, norm_gain,
    routes, route_weight, expert_gate, expert_up, expert_down,
):
    n, tp = lax.axis_size("sp"), lax.axis_size("tp")
    tok, feat = resid.shape
    channels = pool_input.shape[1]
    folds = max(1, LANES // channels)
    model, width = expert_gate.shape[1:]
    cap = 2 * tok * TOPK // n
    ny = tp // CORES
    group = min(n, max(1, CHUNK_ROWS // cap))
    chunks = n // group
    rows = group * cap
    sems = pltpu.SemaphoreType.DMA
    vmem = pl.BlockSpec(memory_space=pltpu.VMEM)
    hbm = pl.BlockSpec(memory_space=pl.ANY)
    return pl.pallas_call(
        functools.partial(layer_kernel, n, tp, cap),
        out_shape=pltpu.VMEM((tok, feat), BF16),
        in_specs=[vmem] * 8 + [hbm] * 3,
        out_specs=vmem,
        scratch_shapes=[
            pltpu.VMEM((REACH, folds * channels), BF16),
            pltpu.VMEM((tp, REACH, folds * channels), BF16),
            pltpu.VMEM((tp, tok // folds, folds * channels), BF16),
            pltpu.VMEM((tp, 8, tok), F32),
            pltpu.VMEM((tok, feat), BF16),
            pltpu.VMEM((tok, feat), BF16),
            pltpu.VMEM((n, cap, model), BF16),
            pltpu.VMEM((n, cap, feat), BF16),
            pltpu.VMEM((n, 8, max(cap, LANES)), F32),
            pltpu.VMEM((n, 8, max(cap, LANES)), F32),
            pltpu.VMEM((model, width), BF16),
            pltpu.VMEM((model, width), BF16),
            pltpu.VMEM((width, model), BF16),
            pltpu.VMEM((rows, width), BF16),
            pltpu.VMEM((2, rows, ny * feat), F32),
            pltpu.VMEM((chunks, rows, feat), F32),
            pltpu.VMEM((chunks, rows, ny * feat), BF16),
            pltpu.VMEM((chunks, rows, ny * feat), BF16),
            pltpu.VMEM((chunks, ny, rows, feat), BF16),
            pltpu.VMEM((chunks, ny, rows, feat), BF16),
            pltpu.VMEM((n, cap, feat), BF16),
            pltpu.VMEM((n, cap, feat), BF16),
            pltpu.VMEM((tok, feat), F32),
            sems((3,)),
            sems((tp,)), sems((tp,)),
            sems((tp,)), sems((tp,)),
            sems((tp,)), sems((tp,)),
            sems((n,)), sems((n,)),
            sems((n,)), sems((n,)),
            sems((n, ny)), sems((n, ny)),
            sems((n, ny)), sems((n, ny)),
            sems((chunks,)), sems((chunks,)),
            sems((chunks, ny)), sems((chunks, ny)),
            sems((n,)), sems((n,)),
        ],
        compiler_params=pltpu.CompilerParams(
            collective_id=0, has_side_effects=True, vmem_limit_bytes=56 * 1024 * 1024
        ),
    )(
        pool_input.T, pool_weight, pool_gain.reshape(1, -1), out_weight, resid, norm_gain.reshape(-1, LANES),
        routes.T, route_weight.T, expert_gate, expert_up, expert_down,
    )


def solution(mesh):
    in_specs = (
        P("sp", "tp"),
        P("tp", None, None),
        P("tp"),
        P(None, "tp"),
        P("sp", "tp"),
        P("tp"),
        P("sp", None),
        P("sp", None),
        P("sp", None, "tp"),
        P("sp", None, "tp"),
        P("sp", "tp", None),
    )
    return jax.shard_map(on_device, mesh=mesh, in_specs=in_specs, out_specs=P("sp", "tp"), check_vma=False)
```

```python
import functools

import jax
import jax.numpy as jnp
from jax import lax
from jax.experimental import pallas as pl
from jax.experimental.pallas import tpu as pltpu
from jax.sharding import PartitionSpec as P

GSIZE = 64
REACH = 16
TOPK = 2
CORES = 2
LANES = 128
CHUNK_ROWS = 128
EARLY = 3

VISITS = (0, 1, 4, 3, 5, 6, 7, 2)
SENDS = (1, 2, 3, 4, 7, 5, 6)
STEPS = (
    ("relay", 0), ("gather", 1), ("gate_a", 0), ("gather", 2), ("gate_b", 0), ("down_theirs", 0), ("down_own", 0),
    ("gather", 3), ("pair", 0), ("relay", 1), ("gate_a", 1), ("gate_b", 1), ("reduce", 0), ("relay", 2),
    ("down_theirs", 1), ("down_own", 1), ("gate_a", 2), ("gather", 4), ("gate_b", 2), ("down_theirs", 2),
    ("gather", 7), ("relay", 3), ("pair", 1), ("down_own", 2), ("relay", 4), ("gather", 5), ("gate_a", 3),
    ("pair", 2), ("gate_b", 3), ("down_theirs", 3), ("reduce", 2), ("finish", 0), ("down_own", 3), ("gate_a", 4),
    ("gather", 6), ("gate_b", 4), ("relay", 5), ("down_theirs", 4), ("down_own", 4), ("gate_a", 5), ("finish", 2),
    ("pair", 4), ("reduce", 4), ("gate_b", 5), ("relay", 6), ("down_theirs", 5), ("pair", 3), ("reduce", 3),
    ("down_own", 5), ("relay", 7), ("combine", 0), ("gate_a", 6), ("finish", 4), ("pair", 5), ("reduce", 5),
    ("gate_b", 6), ("reduce", 1), ("down_theirs", 6), ("down_own", 6), ("pair", 6), ("finish", 3), ("gate_a", 7),
    ("gate_b", 7), ("down_theirs", 7), ("reduce", 6), ("finish", 5), ("down_own", 7), ("finish", 1), ("pair", 7),
    ("reduce", 7), ("finish", 6), ("combine", 3), ("combine", 4), ("combine", 1), ("finish", 7), ("combine", 2),
    ("combine", 5), ("combine", 6), ("combine", 7),
)

GATE_LIMIT = 7.0
GATE_ALPHA = 1.702
NORM_EPS = 1e-05

F32 = jnp.float32
BF16 = jnp.bfloat16
MESH = pl.DeviceIdType.MESH


def dot(a, b):
    return jnp.dot(a, b, preferred_element_type=F32)


def visiting_order(chunks, group):
    order, sends, steps = VISITS, SENDS, STEPS
    if chunks != len(VISITS):
        order, sends, steps = range(chunks), range(1, chunks), [("relay", 0)]
        for q in range(chunks):
            steps += [(name, p) for name, p in (("gather", q + 1), ("relay", q + 1)) if p < chunks]
            steps += [(name, q) for name in ("gate_a", "gate_b", "down_theirs", "down_own", "pair", "reduce")]
        steps += [("finish", q) for q in range(chunks)] + [("combine", q) for q in range(chunks)]
    offsets = [q * group + j for q in order for j in range(group)]
    sending = [*range(1, group)] + [q * group + j for q in sends for j in range(group)]
    return offsets, sending, steps


def flipped(index, bits):
    bit = 1
    while bit <= bits:
        if bits & bit:
            index = index + bit * (1 - 2 * lax.rem(index // bit, 2))
        bit *= 2
    return index


def windows(summed, level):
    rows, channels = summed.shape
    window, span = jnp.zeros((rows - REACH, channels), F32), jnp.zeros((1, channels), F32)
    for power in range(4):
        summed = summed + pltpu.roll(summed, 1 << power, 0)
        window = jnp.where(level == power, summed[REACH:], window)
        span = jnp.where(level == power, float(2 << power), span)
    return window, span


def layer_kernel(
    n, tp, cap,
    pool_hbm, mix_hbm, gain_hbm, proj_hbm, resid_hbm, norm_hbm, routes_hbm, weight_hbm, gate_hbm, up_hbm, down_hbm,
    out_ref,
    pool_ref, mix_ref, gain_ref, proj_ref, resid_ref, norm_ref, routes_ref, weight_ref,
    edge, edges, packed, squares, stream_ref, normed_ref,
    x, sent, row_send, row_recv, wg, wu, wd, hidden, own, mine, pc_send, pc_recv, ys_send, ys_recv, res, ret, acc,
    i_sem, w_sem, h_send, h_recv, m_send, m_recv, s_send, s_recv, g_send, g_recv, a_send, a_recv, b_send, b_recv, c_send, c_recv, d_send, d_recv, e_send, e_recv, f_send, f_recv,
):
    ny = tp // CORES
    tok, feat = resid_ref.shape
    channels = pool_ref.shape[0]
    model, width = wg.shape
    group = x.shape[0] // ys_send.shape[0]
    chunks = n // group
    rows = group * cap
    order, sending, steps = visiting_order(chunks, group)
    early = group - 1 + EARLY * group
    sp = lax.axis_index("sp")
    t = lax.axis_index("tp")
    y, core = t // CORES, t % CORES
    partner = y * CORES + (1 - core)
    other = [flipped(sp, d) for d in order]

    loads = [
        pltpu.make_async_copy(gate_hbm.at[0], wg, w_sem.at[0]),
        pltpu.make_async_copy(up_hbm.at[0], wu, w_sem.at[1]),
        pltpu.make_async_copy(down_hbm.at[0], wd, w_sem.at[2]),
    ]
    fetches = [
        pltpu.make_async_copy(source, target, i_sem.at[i])
        for i, (source, target) in enumerate([
            (pool_hbm, pool_ref), (mix_hbm, mix_ref), (gain_hbm, gain_ref), (routes_hbm, routes_ref),
            (weight_hbm, weight_ref), (resid_hbm, resid_ref), (proj_hbm, proj_ref), (norm_hbm, norm_ref),
        ])
    ]
    for fetch in fetches:
        fetch.start()

    barrier = pltpu.get_barrier_semaphore()
    after, before = lax.rem(sp + 1, n), lax.rem(sp + n - 1, n)
    peers = [(other[i], t) for i in range(1, n)]
    peers += [(sp, lax.rem(t + k, tp)) for k in range(1, tp)]
    peers += [(s, lax.rem(t + k, tp)) for s in (after, before) for k in range(1, tp)]
    for peer in peers:
        pl.semaphore_signal(barrier, inc=1, device_id=peer, device_id_type=MESH)
    for load in loads:
        load.start()
    for fetch in fetches:
        fetch.wait()

    def cols(block):
        return pl.ds(pl.multiple_of(block * feat, LANES), feat)

    def remote(src, dst, send, recv, device):
        return pltpu.make_async_remote_copy(
            src_ref=src, dst_ref=dst, send_sem=send, recv_sem=recv, device_id=device, device_id_type=MESH
        )

    def copy_a(i):
        return remote(sent.at[i], x.at[i, :, cols(t)], a_send.at[i], a_recv.at[i], (other[i], t))

    def copy_g(i):
        return remote(row_send.at[i], row_recv.at[i], g_send.at[i], g_recv.at[i], (other[i], t))

    def copy_b(i, k):
        part = x.at[i, :, cols(t)]
        return remote(part, part, b_send.at[i, k], b_recv.at[i, k], (sp, lax.rem(y + k, ny) * CORES + core))

    def copy_c(i, k):
        part = x.at[i, :, cols(lax.rem(y + ny - k, ny) * CORES + core)]
        return remote(part, part, c_send.at[i, k], c_recv.at[i, k], (sp, partner))

    def copy_d(q):
        return remote(pc_send.at[q], pc_recv.at[q], d_send.at[q], d_recv.at[q], (sp, partner))

    def copy_e(q, k):
        return remote(
            ys_send.at[q, k], ys_recv.at[q, k], e_send.at[q, k], e_recv.at[q, k],
            (sp, lax.rem(y + k, ny) * CORES + core),
        )

    def copy_f(i):
        return remote(res.at[i], ret.at[i], f_send.at[i], f_recv.at[i], (other[i], t))

    def copy_h(k):
        return remote(edge, edges.at[k], h_send.at[k], h_recv.at[k], (after, lax.rem(t + k, tp)))

    def copy_m(k):
        return remote(packed.at[0], packed.at[k], m_send.at[k], m_recv.at[k], (sp, lax.rem(t + k, tp)))

    def copy_s(k):
        return remote(squares.at[0], squares.at[k], s_send.at[k], s_recv.at[k], (sp, lax.rem(t + k, tp)))

    with jax.named_scope("local"):
        current = pool_ref[...].astype(F32).T
        groups = channels // GSIZE
        group_of = t * groups + lax.broadcasted_iota(jnp.int32, (1, channels), 1) // GSIZE
        level = lax.rem(group_of, 4)
        blank = jnp.zeros((REACH, channels), F32)
        window, span = windows(jnp.concatenate([blank, current], axis=0), level)
        place = (sp * tok + 1 + lax.broadcasted_iota(jnp.int32, (tok, channels), 0)).astype(F32)
        pooled = (window / jnp.minimum(place, span) - current).astype(BF16)
        carried, _ = windows(jnp.concatenate([current[tok - REACH :], blank], axis=0), level)
        carried = (carried / span).astype(BF16)
        gain = gain_ref[...].astype(F32)

        def mix(values):
            parts = [dot(values[:, g * GSIZE : (g + 1) * GSIZE], mix_ref[g]) for g in range(groups)]
            return (jnp.concatenate(parts, axis=1) * gain).astype(BF16)

        mixed = mix(pooled)
        folds = max(1, LANES // channels)
        short = tok // folds
        packed[0] = jnp.concatenate([mixed[i * short : (i + 1) * short] for i in range(folds)], axis=1)
        edge[...] = jnp.concatenate([mix(carried)] * folds, axis=1)

        listed = jnp.concatenate(
            [routes_ref[...].astype(F32), weight_ref[...], jnp.zeros((8 - 2 * TOPK, tok), F32)], axis=0
        ).T
        routes = [listed[:, k : k + 1] for k in range(TOPK)]
        weights = [listed[:, TOPK + k : TOPK + k + 1] for k in range(TOPK)]
        lane = lax.broadcasted_iota(jnp.int32, (tok, LANES), 1).astype(F32)
        onehot = [jnp.where(route == lane, 1.0, 0.0) for route in routes]
        below = lax.broadcasted_iota(jnp.int32, (tok, tok), 1) < lax.broadcasted_iota(jnp.int32, (tok, tok), 0)
        earlier = dot(jnp.where(below, 1.0, 0.0).astype(BF16), sum(onehot).astype(BF16))
        keys = [
            routes[k] * float(cap) + jnp.sum(earlier * onehot[k], axis=1, keepdims=True) for k in range(TOPK)
        ]
        slot = lax.broadcasted_iota(jnp.int32, (tok, cap), 1)
        acc[...] = resid_ref[...].astype(F32)

    with jax.named_scope("barrier"):
        pl.semaphore_wait(barrier, len(peers))
    for k in range(1, tp):
        copy_m(k).start()

    @pl.when(sp < n - 1)
    def _():
        for k in range(tp):
            copy_h(k).start()

    def projected(block, k):
        first = lax.rem(t + tp - k, tp) * channels
        return dot(block, proj_ref[pl.ds(pl.multiple_of(first, GSIZE), channels), :])

    def unpacked(k):
        block = packed[k]
        return jnp.concatenate([block[:, i * channels : (i + 1) * channels] for i in range(folds)], axis=0)

    with jax.named_scope("proj"):
        acc[...] += projected(unpacked(0), 0)
        for k in range(1, tp):
            copy_m(k).wait_recv()
            acc[...] += projected(unpacked(k), k)

    with jax.named_scope("halo"):
        @pl.when(sp > 0)
        def _():
            for k in range(tp):
                copy_h(k).wait_recv()
                acc[:REACH] += projected(edges[k][:, :channels], k)

    with jax.named_scope("stream"):
        stream_ref[...] = acc[...].astype(BF16)
        stream = stream_ref[...].astype(F32)
        power = jnp.sum(stream * stream, axis=1, keepdims=True)
        squares[0] = jnp.broadcast_to(power, (tok, LANES)).T[:8]
        for k in range(1, tp):
            copy_s(k).start()
        scaling = norm_ref[...].astype(F32)
        scaling = jnp.concatenate([scaling[i : i + 1] for i in range(feat // LANES)], axis=1)
        normed_ref[...] = (stream * scaling).astype(BF16)

    def chosen(i):
        wanted = (slot + other[i] * cap).astype(F32)
        return sum(jnp.where(key == wanted, 1.0, 0.0) for key in keys)

    def rows_for(i):
        return lax.dot_general(
            chosen(i).astype(BF16), normed_ref[...], (((0,), (0,)), ((), ())), preferred_element_type=F32
        ).astype(BF16)

    def arrive_a(i):
        if i:
            copy_a(i).wait_recv()
        for k in range(1, ny):
            copy_b(i, k).start()
        copy_c(i, 0).start()

    def arrive_b(i):
        for k in range(1, ny):
            copy_b(i, k).wait_recv()
            copy_c(i, k).start()

    def arrive_c(i):
        for k in range(ny):
            copy_c(i, k).wait_recv()

    def dispatch(first, last):
        for i in sending[first:last]:
            sent[i] = rows_for(i)
            copy_a(i).start()

    with jax.named_scope("dispatch"):
        x[0, :, cols(t)] = rows_for(0)
        arrive_a(0)
        dispatch(0, early)

    with jax.named_scope("scales"):
        total = squares[0]
        for k in range(1, tp):
            copy_s(k).wait_recv()
            total = total + squares[k]
        scale = lax.rsqrt(total.T[:, :1] / model + NORM_EPS)
        for i in range(n):
            line = jnp.sum(chosen(i) * scale, axis=0, keepdims=True)
            if cap < LANES:
                line = jnp.concatenate([line, jnp.zeros((1, LANES - cap), F32)], axis=1)
            if i:
                row_send[i] = jnp.broadcast_to(line, row_send.shape[1:])
                copy_g(i).start()
            else:
                row_recv[0] = jnp.broadcast_to(line, row_send.shape[1:])
        dispatch(early, n)

    def members(q):
        return range(q * group, (q + 1) * group) if q < chunks else ()

    def gather(q):
        for i in members(q):
            arrive_a(i)

    def relay(q):
        for i in members(q):
            arrive_b(i)

    step = min(width, 256)

    def gate_up(q, first, last):
        scaled = jnp.concatenate([row_recv[i].T[:cap, :1] for i in members(q)], axis=0)

        @pl.loop(first, last)
        def _(j):
            part = pl.ds(pl.multiple_of(j * step, LANES), step)
            block = x[q * group : (q + 1) * group].reshape(rows, model)
            gate = jnp.minimum(dot(block, wg[:, part]) * scaled, GATE_LIMIT)
            up = jnp.clip(dot(block, wu[:, part]) * scaled, -GATE_LIMIT, GATE_LIMIT)
            hidden[:, part] = ((up + 1.0) * gate * jax.nn.sigmoid(GATE_ALPHA * gate)).astype(BF16)

    def gate_a(q):
        for i in members(q):
            arrive_c(i)
            if i:
                copy_g(i).wait_recv()
        if q == 0:
            loads[0].wait()
            loads[1].wait()
        gate_up(q, 0, width // step // 2)

    def gate_b(q):
        gate_up(q, width // step // 2, width // step)

    def down_theirs(q):
        if q == 0:
            loads[2].wait()
        for k in range(ny):
            block = lax.rem(y + k, ny) * CORES + (1 - core)
            pc_send[q, :, k * feat : (k + 1) * feat] = dot(hidden[...], wd[:, cols(block)]).astype(BF16)
        copy_d(q).start()

    def down_own(q):
        for k in range(ny):
            block = lax.rem(y + k, ny) * CORES + core
            own[q % 2, :, k * feat : (k + 1) * feat] = dot(hidden[...], wd[:, cols(block)])

    def pair(q):
        copy_d(q).wait_recv()
        for k in range(1, ny):
            part = slice(k * feat, (k + 1) * feat)
            ys_send[q, k] = (own[q % 2, :, part] + pc_recv[q, :, part].astype(F32)).astype(BF16)
        mine[q] = own[q % 2, :, :feat] + pc_recv[q, :, :feat].astype(F32)

    def reduce(q):
        for k in range(1, ny):
            copy_e(q, k).start()

    def finish(q):
        total = mine[q]
        for k in range(1, ny):
            copy_e(q, k).wait_recv()
            total = total + ys_recv[q, k].astype(F32)
        total = total.astype(BF16)
        for j in range(group):
            i = q * group + j
            block = total[j * cap : (j + 1) * cap]
            if i:
                res[i] = block
                copy_f(i).start()
            else:
                ret[0] = block

    heads = [weight.astype(BF16).astype(F32) for weight in weights]
    rests = [weights[k] - heads[k] for k in range(TOPK)]

    def combine(q):
        for i in members(q):
            if i:
                copy_f(i).wait_recv()
            wanted = (slot + other[i] * cap).astype(F32)
            high = sum(jnp.where(keys[k] == wanted, heads[k], 0.0) for k in range(TOPK))
            low = sum(jnp.where(keys[k] == wanted, rests[k], 0.0) for k in range(TOPK))
            block = ret[i]
            acc[...] += dot(high.astype(BF16), block) + dot(low.astype(BF16), block)

    acc[...] = stream_ref[...].astype(F32)
    actions = dict(
        gather=gather, relay=relay, gate_a=gate_a, gate_b=gate_b, down_theirs=down_theirs, down_own=down_own,
        pair=pair, reduce=reduce, finish=finish, combine=combine,
    )
    for i in members(0):
        if i:
            arrive_a(i)
    for name, q in steps:
        with jax.named_scope(name + str(q)):
            actions[name](q)
    with jax.named_scope("out"):
        out_ref[...] = acc[...].astype(BF16)

    @pl.when(sp < n - 1)
    def _():
        for k in range(tp):
            copy_h(k).wait_send()

    for k in range(1, tp):
        copy_m(k).wait_send()
        copy_s(k).wait_send()
    for i in range(n):
        if i:
            copy_a(i).wait_send()
            copy_g(i).wait_send()
            copy_f(i).wait_send()
        for k in range(ny):
            if k:
                copy_b(i, k).wait_send()
            copy_c(i, k).wait_send()
    for q in range(chunks):
        copy_d(q).wait_send()
        for k in range(1, ny):
            copy_e(q, k).wait_send()


def on_device(
    pool_input, pool_weight, pool_gain, out_weight, resid, norm_gain,
    routes, route_weight, expert_gate, expert_up, expert_down,
):
    n, tp = lax.axis_size("sp"), lax.axis_size("tp")
    tok, feat = resid.shape
    channels = pool_input.shape[1]
    folds = max(1, LANES // channels)
    model, width = expert_gate.shape[1:]
    cap = 2 * tok * TOPK // n
    ny = tp // CORES
    group = min(n, max(1, CHUNK_ROWS // cap))
    chunks = n // group
    rows = group * cap
    sems = pltpu.SemaphoreType.DMA
    vmem = pl.BlockSpec(memory_space=pltpu.VMEM)
    hbm = pl.BlockSpec(memory_space=pl.ANY)
    operands = (
        pool_input.T, pool_weight, pool_gain.reshape(1, -1), out_weight, resid, norm_gain.reshape(-1, LANES),
        routes.T, route_weight.T, expert_gate, expert_up, expert_down,
    )
    return pl.pallas_call(
        functools.partial(layer_kernel, n, tp, cap),
        out_shape=pltpu.VMEM((tok, feat), BF16),
        in_specs=[hbm] * len(operands),
        out_specs=vmem,
        scratch_shapes=[pltpu.VMEM(operand.shape, operand.dtype) for operand in operands[:8]]
        + [
            pltpu.VMEM((REACH, folds * channels), BF16),
            pltpu.VMEM((tp, REACH, folds * channels), BF16),
            pltpu.VMEM((tp, tok // folds, folds * channels), BF16),
            pltpu.VMEM((tp, 8, tok), F32),
            pltpu.VMEM((tok, feat), BF16),
            pltpu.VMEM((tok, feat), BF16),
            pltpu.VMEM((n, cap, model), BF16),
            pltpu.VMEM((n, cap, feat), BF16),
            pltpu.VMEM((n, 8, max(cap, LANES)), F32),
            pltpu.VMEM((n, 8, max(cap, LANES)), F32),
            pltpu.VMEM((model, width), BF16),
            pltpu.VMEM((model, width), BF16),
            pltpu.VMEM((width, model), BF16),
            pltpu.VMEM((rows, width), BF16),
            pltpu.VMEM((2, rows, ny * feat), F32),
            pltpu.VMEM((chunks, rows, feat), F32),
            pltpu.VMEM((chunks, rows, ny * feat), BF16),
            pltpu.VMEM((chunks, rows, ny * feat), BF16),
            pltpu.VMEM((chunks, ny, rows, feat), BF16),
            pltpu.VMEM((chunks, ny, rows, feat), BF16),
            pltpu.VMEM((n, cap, feat), BF16),
            pltpu.VMEM((n, cap, feat), BF16),
            pltpu.VMEM((tok, feat), F32),
            sems((8,)),
            sems((3,)),
            sems((tp,)), sems((tp,)),
            sems((tp,)), sems((tp,)),
            sems((tp,)), sems((tp,)),
            sems((n,)), sems((n,)),
            sems((n,)), sems((n,)),
            sems((n, ny)), sems((n, ny)),
            sems((n, ny)), sems((n, ny)),
            sems((chunks,)), sems((chunks,)),
            sems((chunks, ny)), sems((chunks, ny)),
            sems((n,)), sems((n,)),
        ],
        compiler_params=pltpu.CompilerParams(
            collective_id=0, has_side_effects=True, vmem_limit_bytes=56 * 1024 * 1024
        ),
    )(*operands)


def solution(mesh):
    in_specs = (
        P("sp", "tp"),
        P("tp", None, None),
        P("tp"),
        P(None, "tp"),
        P("sp", "tp"),
        P("tp"),
        P("sp", None),
        P("sp", None),
        P("sp", None, "tp"),
        P("sp", None, "tp"),
        P("sp", "tp", None),
    )
    return jax.shard_map(on_device, mesh=mesh, in_specs=in_specs, out_specs=P("sp", "tp"), check_vma=False)
```
